128 devices in a mesh: tp: 16 (over z, x), dp: 8 (over y, core).
Axes of the slice: x: 4, y: 4, z: 4, core: 2. Of those that a mesh axis runs over, the one named last changes fastest.
Arguments:
- stream_in: bfloat16 [256, 4096], P('tp', 'dp'), may hold values from -21 to 21
- hidden_state: float32 [2, 256, 4096], P(None, 'dp', 'tp'), may hold values from -6 to 6
- convolution_window_state: bfloat16 [2, 256, 3, 4096], P(None, 'dp', None, 'tp'), may hold values from -6 to 6
- norm_gain: float32 [2, 4096], P(None, 'dp'), may hold values from 0.1 to 1.9
- path_weight: bfloat16 [2, 4096, 4096], P(None, 'dp', 'tp'), may hold values from -0.09375 to 0.09375
- output_gate_weight: bfloat16 [2, 4096, 4096], P(None, 'dp', 'tp'), may hold values from -0.09375 to 0.09375
- conv_taps: float32 [2, 4, 4096], P(None, None, 'tp'), may hold values from -3 to 3
- recur_map: float32 [2, 64, 64, 64], P(None, 'tp'), may hold values from -0.75 to 0.75
- input_map: float32 [2, 64, 64, 64], P(None, 'tp'), may hold values from -0.75 to 0.75
- decay_logit: float32 [2, 4096], P(None, 'tp'), may hold values from 1 to 6
- out_weight: bfloat16 [2, 4096, 4096], P(None, 'tp', 'dp'), may hold values from -0.09375 to 0.09375
Outputs:
- stream_out: bfloat16 [256, 4096], P('tp', 'dp')
- hidden_next: float32 [2, 256, 4096], P(None, 'dp', 'tp')
- conv_next: bfloat16 [2, 256, 3, 4096], P(None, 'dp', None, 'tp')
The draws below stay inside these ranges and needn't reach their ends.
All inputs are finite; a program needn't handle non-finite values.
Results may differ from the reference program's by a relative error of at most 0.019.
Values may be sent and summed in bfloat16 or wider, within the bound.
A program may use at most 64 MiB of HBM per device.

```python
import jax
import jax.numpy as jnp
from jax import lax

D = 4096
R = 4096
BLOCK_W = 64
NBLK = 64
LAYERS = 2
TAPS = 4
BATCH = 256
N_DP = 8


def draw_stream_in(key, part):
    first, second = jax.random.split(key, 2)
    groups = D // 64
    group_scale = jnp.exp(jax.random.uniform(first, (groups,), jnp.float32, jnp.log(0.3), jnp.log(3.0)))
    column_scale = jnp.repeat(group_scale, 64)
    values = jnp.clip(jax.random.normal(second, (BATCH, D), jnp.float32), -4.0, 4.0)
    return (values * column_scale[None, :]).astype(jnp.bfloat16)


def level_of(rng, dims, cuts, low, largest):
    loudness = 1.0
    for axis_at, shards_of in cuts:
        steps = jax.random.uniform(jax.random.fold_in(jax.random.fold_in(rng, 6), axis_at), (shards_of,), jnp.float32, low / len(cuts), largest / len(cuts))
        loudness = loudness * jnp.repeat(jnp.exp(steps), dims[axis_at] // shards_of).reshape((-1,) + (1,) * (len(dims) - 1 - axis_at))
    return loudness


def scatter_about(rng, extent, scale, most, shards=(), dtype=jnp.bfloat16):
    factor_of = level_of(rng, extent, shards, -0.22, 0.18) if shards else 1.0
    drawn = jax.random.normal(rng, extent, jnp.float32) * scale * factor_of
    return jnp.minimum(jnp.maximum(drawn, -most), most).astype(dtype)


def setup_inputs(seed: int = 0) -> dict:
    streams_of = jax.random.split(jax.random.key(seed), 12)
    return {
        "stream_in": draw_stream_in(jax.random.fold_in(streams_of[11], 71), 0),
        "hidden_state": scatter_about(streams_of[1], (LAYERS, BATCH, R), 1.0, 6.0, ((1, 8), (2, 16)), jnp.float32),
        "convolution_window_state": scatter_about(streams_of[2], (LAYERS, BATCH, TAPS - 1, R), 1.0, 6.0, ((1, 8), (3, 16))),
        "norm_gain": jnp.clip(1.0 + 0.18 * jax.random.normal(streams_of[3], (LAYERS, D), jnp.float32), 0.1, 1.9),
        "path_weight": scatter_about(streams_of[4], (LAYERS, D, R), D ** -0.5, 0.09375, ((1, 8), (2, 16))),
        "output_gate_weight": scatter_about(streams_of[5], (LAYERS, D, R), D ** -0.5, 0.09375, ((1, 8), (2, 16))),
        "conv_taps": scatter_about(streams_of[6], (LAYERS, TAPS, R), 0.5, 3.0, ((2, 16),), jnp.float32),
        "recur_map": scatter_about(streams_of[7], (LAYERS, NBLK, BLOCK_W, BLOCK_W), BLOCK_W ** -0.5, 0.75, ((1, 16),), jnp.float32),
        "input_map": scatter_about(streams_of[8], (LAYERS, NBLK, BLOCK_W, BLOCK_W), BLOCK_W ** -0.5, 0.75, ((1, 16),), jnp.float32),
        "decay_logit": jnp.clip(1.0 + 5.0 * jax.random.uniform(streams_of[9], (LAYERS, R), jnp.float32) ** level_of(streams_of[9], (LAYERS, R), ((1, 16),), -0.2, 0.2), 1.0, 6.0),
        "out_weight": scatter_about(streams_of[10], (LAYERS, R, D), R ** -0.5, 0.09375, ((1, 16), (2, 8))),
    }


EPS = 1e-06

def one_block(stream, hidden, buffer, gain, path_w, gate_branch_matrix, taps, recur_w, input_matrix, logit, out_w):
    batch = stream.shape[0]
    streamf = stream.astype(jnp.float32)
    sumsq = lax.optimization_barrier(jnp.sum(streamf * streamf, axis=1))
    normed = (streamf * lax.rsqrt(sumsq / D + EPS)[:, None] * gain[None, :]).astype(jnp.bfloat16)
    block_list = normed.astype(jnp.float32).reshape(batch, N_DP, D // N_DP)

    def summed(weight):
        weight_block_list = weight.astype(jnp.float32).reshape(N_DP, D // N_DP, R)
        piece_list = jnp.einsum('yiq,iqx->iyx', block_list, weight_block_list).astype(jnp.bfloat16)
        piece_list = lax.optimization_barrier(piece_list).astype(jnp.float32)
        return lax.optimization_barrier(jnp.sum(piece_list, axis=0)).astype(jnp.bfloat16)
    zpath = summed(path_w)
    zgate = summed(gate_branch_matrix)
    conv = zpath.astype(jnp.float32) * taps[TAPS - 1][None, :]
    for j in range(TAPS - 1):
        conv = conv + buffer[:, j].astype(jnp.float32) * taps[j][None, :]
    new_buffer = jnp.concatenate([buffer[:, 1:], zpath[:, None, :]], axis=1)
    cblocks = conv.reshape(batch, NBLK, BLOCK_W)
    rgate = jax.nn.sigmoid(jnp.einsum('bnc,ncd->bnd', cblocks, recur_w, precision=lax.Precision.HIGHEST).reshape(batch, R))
    igate = jax.nn.sigmoid(jnp.einsum('bnc,ncd->bnd', cblocks, input_matrix, precision=lax.Precision.HIGHEST).reshape(batch, R))
    loga = 8.0 * rgate * jax.nn.log_sigmoid(logit)[None, :]
    new_hidden = jnp.exp(loga) * hidden + jnp.sqrt(-jnp.expm1(2.0 * loga)) * (igate * conv)
    mixed = (new_hidden * jax.nn.gelu(zgate.astype(jnp.float32))).astype(jnp.bfloat16)
    update = jnp.dot(mixed, out_w, preferred_element_type=jnp.float32)
    return ((streamf + update).astype(jnp.bfloat16), new_hidden, new_buffer)

def reference(stream_in, hidden_state, convolution_window_state, norm_gain, path_weight, output_gate_weight, conv_taps, recur_map, input_map, decay_logit, out_weight):
    stream = stream_in
    hiddens = []
    buffers = []
    for layer in range(LAYERS):
        stream, new_hidden, new_buffer = one_block(stream, hidden_state[layer], convolution_window_state[layer], norm_gain[layer], path_weight[layer], output_gate_weight[layer], conv_taps[layer], recur_map[layer], input_map[layer], decay_logit[layer], out_weight[layer])
        hiddens.append(new_hidden)
        buffers.append(new_buffer)
    return (stream, jnp.stack(hiddens), jnp.stack(buffers))
```

```python
import functools

import jax
import jax.numpy as jnp
from jax import lax
from jax.experimental import pallas as pl
from jax.experimental.pallas import tpu as pltpu
from jax.sharding import PartitionSpec as P

D = 4096
TAPS = 4
EPS = 1e-06
LAYERS = 2
NZ, NX, NY, NC = 4, 4, 4, 2
TP, DP = NZ * NX, NY * NC
ROWS = 16
SROWS = 32
DLOC = 512
W = 256
MESH = pl.DeviceIdType.MESH
f32, bf16 = jnp.float32, jnp.bfloat16


def near(k):
    half = lax.div(k, 2)
    return k + half * (1 - 2 * lax.rem(k, 2))


def kernel(x_h, hid_h, buf_h, gain_h, pw_h, gw_h, taps_h, rmap_h, imap_h, logit_h, ow_h,
           so_ref, ho_ref, bo_ref,
           xg, wz, wo, hid, buf, gain, taps, logit, rmap, imap, bdh, bdl, pre, la,
           zs, zr, sss, ssr, ms, mg, us, ur,
           lsem, xss, xrs, zss, zrs, qss, qrs, mss, mrs, uss, urs):
    tp = lax.axis_index("tp")
    dp = lax.axis_index("dp")
    z0, x0 = lax.div(tp, NX), lax.rem(tp, NX)
    y0, c0 = lax.div(dp, NC), lax.rem(dp, NC)

    def tp_at(i):
        z = lax.rem(z0 + near(lax.div(i, 4)), NZ)
        x = lax.rem(x0 + near(lax.rem(i, 4)), NX)
        return z * NX + x

    def dp_at(i):
        y = lax.rem(y0 + near(lax.div(i, 2)), NY)
        c = lax.rem(c0 + lax.rem(i, 2), NC)
        return y * NC + c

    def group_at(i):
        z = lax.rem(z0 + near(lax.div(i, 2)), NZ)
        p = lax.rem(lax.div(x0, 2) + lax.rem(i, 2), 2)
        return z * 2 + p

    loads = [
        (x_h, xg.at[0, tp]),
        (gain_h, gain),
        (pw_h.at[0], wz.at[0, :, pl.ds(0, W)]),
        (gw_h.at[0], wz.at[0, :, pl.ds(W, W)]),
        (buf_h, buf),
        (taps_h, taps),
        (logit_h, logit),
        (rmap_h, rmap),
        (imap_h, imap),
        (hid_h, hid),
        (ow_h.at[0], wo.at[0]),
        (pw_h.at[1], wz.at[1, :, pl.ds(0, W)]),
        (gw_h.at[1], wz.at[1, :, pl.ds(W, W)]),
        (ow_h.at[1], wo.at[1]),
    ]
    copies = [pltpu.make_async_copy(a, b, lsem.at[i]) for i, (a, b) in enumerate(loads)]
    for c in copies:
        c.start()

    barrier = pltpu.get_barrier_semaphore()

    def greet_tp(i, _):
        pl.semaphore_signal(barrier, inc=1, device_id={"tp": tp_at(TP - i), "dp": dp}, device_id_type=MESH)
        return 0

    def greet_dp(i, _):
        pl.semaphore_signal(barrier, inc=1, device_id={"tp": tp, "dp": dp_at(DP - i)}, device_id_type=MESH)
        return 0

    lax.fori_loop(1, TP, greet_tp, 0)
    lax.fori_loop(1, DP, greet_dp, 0)

    for i in (4, 5, 6, 7, 8):
        copies[i].wait()
    la[...] = 8.0 * jax.nn.log_sigmoid(logit[...])
    for l in range(LAYERS):
        acc = buf[l, 0].astype(f32) * taps[l, 0:1, :]
        for j in range(1, TAPS - 1):
            acc = acc + buf[l, j].astype(f32) * taps[l, j : j + 1, :]
        pre[l] = acc
        bo_ref[l, 0] = buf[l, 1]
        bo_ref[l, 1] = buf[l, 2]
        zero = jnp.zeros((64, 64), f32)
        zpair = jnp.zeros((64, 128), bf16)
        for b in range(4):
            for m, ref in enumerate((rmap, imap)):
                block = ref[l, b]
                wide = jnp.concatenate([block, zero] if b % 2 == 0 else [zero, block], axis=1)
                hi = wide.astype(bf16)
                lo = (wide - hi.astype(f32)).astype(bf16)
                for h in range(2):
                    at = pl.ds(m * W + h * 128, 128)
                    here = h == b // 2
                    bdh[l, b * 64 : b * 64 + 64, at] = hi if here else zpair
                    bdl[l, b * 64 : b * 64 + 64, at] = lo if here else zpair

    copies[0].wait()
    pl.semaphore_wait(barrier, TP - 1 + DP - 1)

    def x_copy(l, t, slot):
        return pltpu.make_async_remote_copy(
            src_ref=xg.at[l, tp], dst_ref=xg.at[l, slot],
            send_sem=xss.at[l, t], recv_sem=xrs.at[l, slot],
            device_id={"tp": t, "dp": dp}, device_id_type=MESH)

    def z_copy(l, d, slot):
        return pltpu.make_async_remote_copy(
            src_ref=zs.at[l, d], dst_ref=zr.at[l, slot],
            send_sem=zss.at[l, d], recv_sem=zrs.at[l, slot],
            device_id={"tp": tp, "dp": d}, device_id_type=MESH)

    def q_copy(l, d, slot):
        return pltpu.make_async_remote_copy(
            src_ref=sss.at[l, d], dst_ref=ssr.at[l, slot],
            send_sem=qss.at[l, d], recv_sem=qrs.at[l, slot],
            device_id={"tp": tp, "dp": d}, device_id_type=MESH)

    def m_copy(l, d, slot):
        return pltpu.make_async_remote_copy(
            src_ref=ms.at[l], dst_ref=mg.at[l, slot],
            send_sem=mss.at[l, d], recv_sem=mrs.at[l, slot],
            device_id={"tp": tp, "dp": d}, device_id_type=MESH)

    def u_copy(l, t, slot):
        return pltpu.make_async_remote_copy(
            src_ref=us.at[l, t], dst_ref=ur.at[l, slot],
            send_sem=uss.at[l, t], recv_sem=urs.at[l, slot],
            device_id={"tp": t, "dp": dp}, device_id_type=MESH)

    eye = (lax.broadcasted_iota(jnp.int32, (SROWS, 128), 0)
           == lax.broadcasted_iota(jnp.int32, (SROWS, 128), 1))

    for l in range(LAYERS):
        def send_x(i, _):
            x_copy(l, tp_at(TP - i), tp).start()
            return 0

        lax.fori_loop(1, TP, send_x, 0)
        if l == 0:
            for i in (1, 2, 3):
                copies[i].wait()
        else:
            copies[11].wait()
            copies[12].wait()

        def project(i, _):
            g = group_at(i)
            for h in range(2):
                t = 2 * g + h

                @pl.when(t != tp)
                def _():
                    x_copy(l, t, t).wait_recv()

            xf = xg[l, pl.ds(2 * g, 2)].astype(f32).reshape(SROWS, DLOC)
            xn = (xf * gain[l : l + 1, :]).astype(bf16)
            zs[l, g] = jnp.dot(xn, wz[l], preferred_element_type=f32).astype(bf16)
            sq = xf * xf
            sq = (sq[:, 0:128] + sq[:, 128:256]) + (sq[:, 256:384] + sq[:, 384:512])
            tot = jnp.sum(sq, axis=1, keepdims=True)
            sss[l, g] = jnp.sum(jnp.where(eye, tot, 0.0), axis=0, keepdims=True)

            @pl.when(g != dp)
            def _():
                z_copy(l, g, dp).start()
                q_copy(l, g, dp).start()

            return 0

        lax.fori_loop(0, DP, project, 0)

        if l == 0:
            copies[9].wait()
        acc = zs[l, dp].astype(f32)
        ssum = sss[l, dp]
        for i in range(1, DP):
            d = dp_at(jnp.int32(i))
            z_copy(l, d, d).wait_recv()
            q_copy(l, d, d).wait_recv()
            acc = acc + zr[l, d].astype(f32)
            ssum = ssum + ssr[l, d]
        ss = jnp.sum(jnp.where(eye, ssum, 0.0), axis=1, keepdims=True)
        acc = acc * lax.rsqrt(ss / D + EPS)
        zp = acc[:, :W].astype(bf16)
        zg = acc[:, W:].astype(bf16).astype(f32)

        conv = pre[l] + zp.astype(f32) * taps[l, TAPS - 1 : TAPS, :]
        ch = conv.astype(bf16)
        cl = (conv - ch.astype(f32)).astype(bf16)
        gates = (jnp.dot(ch, bdh[l], preferred_element_type=f32)
                 + jnp.dot(cl, bdh[l], preferred_element_type=f32)
                 + jnp.dot(ch, bdl[l], preferred_element_type=f32))
        rg = jax.nn.sigmoid(gates[:, :W])
        ig = jax.nn.sigmoid(gates[:, W:])
        loga = rg * la[l : l + 1, :]
        th = jnp.tanh(loga)
        hn = jnp.exp(loga) * hid[l] + jnp.sqrt(-2.0 * th / (1.0 - th)) * (ig * conv)
        ms[l] = (hn * jax.nn.gelu(zg)).astype(bf16)

        def send_m(i, _):
            m_copy(l, dp_at(DP - i), dp).start()
            return 0

        lax.fori_loop(1, DP, send_m, 0)
        ho_ref[l] = hn
        bo_ref[l, 2] = zp
        copies[10 if l == 0 else 13].wait()

        def emit(d, rows):
            u = jnp.dot(rows, wo[l], preferred_element_type=f32).astype(bf16)
            us[l, pl.ds(2 * d, 2)] = u.reshape(2, ROWS, DLOC)
            for h in range(2):
                t = 2 * d + h

                @pl.when(t != tp)
                def _():
                    u_copy(l, t, tp).start()

        emit(dp, ms[l])

        def update(i, _):
            d = dp_at(i)
            m_copy(l, d, d).wait_recv()
            emit(d, mg[l, d])
            return 0

        lax.fori_loop(1, DP, update, 0)

        acc = xg[l, tp].astype(f32)
        upd = us[l, tp].astype(f32)
        for i in range(1, TP):
            t = tp_at(jnp.int32(i))
            u_copy(l, t, t).wait_recv()
            upd = upd + ur[l, t].astype(f32)
        out = (acc + upd).astype(bf16)
        if l + 1 < LAYERS:
            xg[l + 1, tp] = out
        else:
            so_ref[...] = out

    for l in range(LAYERS):
        def drain_tp(i, _):
            t = tp_at(i)
            x_copy(l, t, tp).wait_send()
            u_copy(l, t, tp).wait_send()
            return 0

        def drain_dp(i, _):
            d = dp_at(i)
            z_copy(l, d, dp).wait_send()
            q_copy(l, d, dp).wait_send()
            m_copy(l, d, dp).wait_send()
            return 0

        lax.fori_loop(1, TP, drain_tp, 0)
        lax.fori_loop(1, DP, drain_dp, 0)


def per_device(*args):
    args = list(args)
    args[2] = jnp.transpose(args[2], (0, 2, 1, 3))
    V = pltpu.VMEM
    S = pltpu.SemaphoreType.DMA
    so, ho, bo = pl.pallas_call(
        kernel,
        out_shape=(
            jax.ShapeDtypeStruct((ROWS, DLOC), bf16),
            jax.ShapeDtypeStruct((LAYERS, SROWS, W), f32),
            jax.ShapeDtypeStruct((LAYERS, TAPS - 1, SROWS, W), bf16),
        ),
        in_specs=[pl.BlockSpec(memory_space=pltpu.HBM)] * 11,
        out_specs=[pl.BlockSpec(memory_space=pltpu.VMEM)] * 3,
        scratch_shapes=[
            V((LAYERS, TP, ROWS, DLOC), bf16),
            V((LAYERS, DLOC, 2 * W), bf16),
            V((LAYERS, W, DLOC), bf16),
            V((LAYERS, SROWS, W), f32),
            V((LAYERS, TAPS - 1, SROWS, W), bf16),
            V((LAYERS, DLOC), f32),
            V((LAYERS, TAPS, W), f32),
            V((LAYERS, W), f32),
            V((LAYERS, 4, 64, 64), f32),
            V((LAYERS, 4, 64, 64), f32),
            V((LAYERS, W, 2 * W), bf16),
            V((LAYERS, W, 2 * W), bf16),
            V((LAYERS, SROWS, W), f32),
            V((LAYERS, W), f32),
            V((LAYERS, DP, SROWS, 2 * W), bf16),
            V((LAYERS, DP, SROWS, 2 * W), bf16),
            V((LAYERS, DP, 1, 128), f32),
            V((LAYERS, DP, 1, 128), f32),
            V((LAYERS, SROWS, W), bf16),
            V((LAYERS, DP, SROWS, W), bf16),
            V((LAYERS, TP, ROWS, DLOC), bf16),
            V((LAYERS, TP, ROWS, DLOC), bf16),
            S((14,)),
            S((LAYERS, TP)), S((LAYERS, TP)),
            S((LAYERS, DP)), S((LAYERS, DP)),
            S((LAYERS, DP)), S((LAYERS, DP)),
            S((LAYERS, DP)), S((LAYERS, DP)),
            S((LAYERS, TP)), S((LAYERS, TP)),
        ],
        compiler_params=pltpu.CompilerParams(
            collective_id=0, has_side_effects=True, vmem_limit_bytes=40 * 1024 * 1024),
        name="blocks",
    )(*args)
    return so, ho, jnp.transpose(bo, (0, 2, 1, 3))


def solution(mesh):
    placed = (
        P("tp", "dp"),
        P(None, "dp", "tp"),
        P(None, "dp", None, "tp"),
        P(None, "dp"),
        P(None, "dp", "tp"),
        P(None, "dp", "tp"),
        P(None, None, "tp"),
        P(None, "tp", None, None),
        P(None, "tp", None, None),
        P(None, "tp"),
        P(None, "tp", "dp"),
    )
    return jax.shard_map(
        per_device,
        mesh=mesh,
        in_specs=placed,
        out_specs=(P("tp", "dp"), P(None, "dp", "tp"), P(None, "dp", None, "tp")),
        check_vma=False,
    )
```
